32 devices in a mesh: ep: 16 (over z, x, core), tp: 2 (over y).
Axes of the slice: x: 2, y: 2, z: 4, core: 2. Of those that a mesh axis runs over, the one named last changes fastest.
Arguments:
- tokens: bfloat16 [192, 4096], P('ep', 'tp')
- norm_gain: float32 [4096], P('tp'), may hold values from 0.1 to 1.9
- routes: int32 [192, 6], P('ep'), may hold values from 0 to 15, all different within a row; in each aligned block of 12 rows (0 to 11, 12 to 23, ...) at most 5 rows name the same one
- route_weights: float32 [192, 6], P('ep'), may hold values from 0.05 to 1
- expert_gate: bfloat16 [16, 4096, 1024], P('ep', 'tp'), may hold values from -0.09375 to 0.09375
- expert_up: bfloat16 [16, 4096, 1024], P('ep', 'tp'), may hold values from -0.09375 to 0.09375
- expert_down: bfloat16 [16, 1024, 4096], P('ep', None, 'tp'), may hold values from -0.1875 to 0.1875
- shared_gate: bfloat16 [4096, 1024], P('tp'), may hold values from -0.09375 to 0.09375
- shared_up: bfloat16 [4096, 1024], P('tp'), may hold values from -0.09375 to 0.09375
- shared_down: bfloat16 [1024, 4096], P(None, 'tp'), may hold values from -0.1875 to 0.1875
Outputs:
- mixed: bfloat16 [192, 4096], P('ep', 'tp')
The draws below stay inside these ranges and needn't reach their ends.
Inputs may be any that keep to these rules, and one draw needn't show every extreme that they name: `routes`: each row names 6 different experts; among the rows of one device no expert is named more than 5 times, and in some devices' rows one expert is named exactly 5 times.
All inputs are finite; a program needn't handle non-finite values.
Results may differ from the reference program's by a relative error of at most 0.0068.
Values may be sent and summed in bfloat16 or wider, within the bound.
A program may use at most 64 MiB of HBM per device.

```python
import math
import jax
import jax.numpy as jnp
import numpy as np
from jax import lax

D = 4096
FF_E = 1024
FF_S = 1024
TOP_K = 6
TOK_DEV = 12
EXPERTS = 16
CAP = 5
TOKENS = 192
N_EP = 16


def draw_tokens(key, part):
    first, second = jax.random.split(jax.random.fold_in(key, 11), 2)
    column = jnp.arange(D, dtype=jnp.float32) / D
    rising = jnp.exp(jnp.log(8.0) * column)[None, :]
    base = jax.random.normal(first, (TOKENS, D), jnp.float32)
    rough = jax.random.uniform(second, (1, D), jnp.float32, 0.5, 1.5)
    values = jnp.clip(base, -6.0, 6.0) * rough * rising
    return values.astype(jnp.bfloat16)


def block_levels(key, shape, cuts, least, high):
    def one(dim, parts):
        steps = jax.random.uniform(jax.random.fold_in(jax.random.fold_in(key, 6), dim), (parts,), jnp.float32, least / len(cuts), high / len(cuts))
        return jnp.repeat(jnp.exp(steps), shape[dim] // parts).reshape((-1,) + (1,) * (len(shape) - dim - 1))

    level = one(*cuts[0])
    for cut in cuts[1:]:
        level = level * one(*cut)
    return level


def deal_out(stream_key, own, number, rows, count, top, limit, lean):
    sequence = jax.random.permutation(stream_key, count)
    heavy_load, common = shares(count, rows * top, limit, lean, True), shares(count, rows * top, limit, lean, False)
    places = jnp.arange(count)

    def named(tallies, offset_by):
        used = int((tallies > 0).sum())
        fixed = max(1, used // 4)
        moved = fixed + (places - fixed + offset_by * (used - fixed)) % max(1, count - fixed)
        return jnp.zeros((count,), jnp.int32).at[sequence[jnp.where(places < fixed, places, moved)]].set(jnp.asarray(tallies, jnp.int32))

    tallies = jnp.where(number % 4 == 0, named(heavy_load, number // 4), named(common, number - number // 4 - 1))
    mixed = jax.random.permutation(jax.random.fold_in(own, 3), count)
    donor, receiver = mixed[0:count // 2 * 2:2], mixed[1:count // 2 * 2:2]
    room = jnp.minimum(tallies[donor] - 1, limit - tallies[receiver]) // 2
    room = jnp.where((donor == sequence[0]) | (receiver == sequence[0]) | (tallies[receiver] == 0), 0, jnp.maximum(room, 0))
    moved = jax.random.randint(jax.random.fold_in(own, 4), (count // 2,), 0, 1 << 20) % (room + 1)
    tallies = tallies.at[donor].add(-moved).at[receiver].add(moved)
    labels = jnp.searchsorted(jnp.cumsum(tallies), jnp.arange(rows * top), side="right").astype(jnp.int32)
    grid = labels.reshape(top, rows).T
    grid = grid[jax.random.permutation(jax.random.fold_in(own, 1), rows)]
    offset_by = jax.random.randint(jax.random.fold_in(own, 2), (rows, 1), 0, top)
    return jnp.take_along_axis(grid, (jnp.arange(top)[None, :] + offset_by) % top, axis=1)


def shares(count, total, most, slope, full):
    weights = [(1 << 20) // math.isqrt(rank ** slope) + 1 for rank in range(1, count + 1)]
    largest = most if full else min(most, max(-(-total // count), total * weights[0] // sum(weights)))
    least = 1 if total - largest >= count - 1 else 0
    given, spare = [largest] + [least] * (count - 1), total - largest - least * (count - 1)
    while spare > 0:
        free = [i for i in range(1, count) if given[i] < largest] or [i for i in range(1, count) if given[i] < most]
        whole, budget = sum([weights[i] for i in free]), spare
        for i in free:
            addition = min(most - given[i], max(1, budget * weights[i] // whole), spare)
            given[i] = given[i] + addition
            spare = spare - addition
    return np.array(given)


def normal_values(own_key, dims, width, bound, cuts=(), held_as=jnp.bfloat16):
    entries = jax.random.normal(own_key, dims, jnp.float32) * width
    if len(cuts) > 0:
        entries = block_levels(own_key, dims, cuts, -0.22, 0.18) * entries
    return jnp.clip(entries, min=-bound, max=bound).astype(held_as)


def setup_inputs(seed: int = 0) -> dict:
    streams_of = jax.random.split(jax.random.key(seed), 11)
    tokens = draw_tokens(jax.random.fold_in(streams_of[10], 71), 0)
    norm_gain = jnp.clip(1.0 + 0.18 * jax.random.normal(streams_of[1], (D,), jnp.float32), 0.1, 1.9)
    routes_keys = jax.random.split(jax.random.fold_in(streams_of[2], 1), TOKENS // TOK_DEV)
    routes_turns = jax.random.permutation(jax.random.fold_in(streams_of[2], 3), TOKENS // TOK_DEV)
    routes = jax.vmap(lambda own, number: deal_out(jax.random.fold_in(streams_of[2], 2), own, number, TOK_DEV, EXPERTS, TOP_K, CAP, 2))(routes_keys, routes_turns).reshape((TOKENS, TOP_K))
    route_weights = jnp.clip(jnp.exp(math.log(1.0) - 2.9957323 * jax.random.uniform(streams_of[3], (TOKENS, TOP_K), jnp.float32) ** block_levels(streams_of[3], (TOKENS, TOP_K), ((0, 16),), -0.2, 0.2)), 0.05, 1.0)
    expert_gate = normal_values(streams_of[4], (EXPERTS, D, FF_E), D ** -0.5, 0.09375, ((0, 16), (1, 2)))
    expert_up = normal_values(streams_of[5], (EXPERTS, D, FF_E), D ** -0.5, 0.09375, ((0, 16), (1, 2)))
    expert_down = normal_values(streams_of[6], (EXPERTS, FF_E, D), FF_E ** -0.5, 0.1875, ((0, 16), (2, 2)))
    shared_gate = normal_values(streams_of[7], (D, FF_S), D ** -0.5, 0.09375, ((0, 2),))
    shared_up = normal_values(streams_of[8], (D, FF_S), D ** -0.5, 0.09375, ((0, 2),))
    shared_down = normal_values(streams_of[9], (FF_S, D), FF_S ** -0.5, 0.1875, ((1, 2),))
    return {"tokens": tokens, "norm_gain": norm_gain, "routes": routes, "route_weights": route_weights, "expert_gate": expert_gate, "expert_up": expert_up, "expert_down": expert_down, "shared_gate": shared_gate, "shared_up": shared_up, "shared_down": shared_down}


def block_ranks(route_blocks, n_experts):
    onehot = (route_blocks[..., None] == jnp.arange(n_experts, dtype=jnp.int32)).astype(jnp.int32)
    before = jnp.cumsum(onehot, axis=1) - onehot
    return lax.optimization_barrier(jnp.sum(before * onehot, axis=-1))

def expert_tables(route_blocks, weight_blocks, expert, capacity, n_experts):
    blocks, tok, picks = route_blocks.shape
    ranks = block_ranks(route_blocks.reshape(blocks, tok * picks), n_experts).reshape(blocks, tok, picks)
    slot = jnp.where(route_blocks == expert, ranks, -1)
    hits = slot[..., None] == jnp.arange(capacity, dtype=jnp.int32)
    select = jnp.any(hits, axis=2).astype(jnp.float32)
    weighted = lax.optimization_barrier(jnp.sum(jnp.where(hits, weight_blocks[..., None], 0.0), axis=2))
    return (select, weighted)

def swiglu(rows, gate_w, up_w, down_w):
    gate = jnp.dot(rows, gate_w, preferred_element_type=jnp.float32)
    up = jnp.dot(rows, up_w, preferred_element_type=jnp.float32)
    hidden = (jax.nn.silu(gate) * up).astype(jnp.bfloat16)
    return jnp.dot(hidden, down_w, preferred_element_type=jnp.float32)

def reference(tokens, norm_gain, routes, route_weights, expert_gate, expert_up, expert_down, shared_gate, shared_up, shared_down):
    values = tokens.astype(jnp.float32)
    meansq = lax.optimization_barrier(jnp.mean(values * values, axis=1, keepdims=True))
    normed = (values * lax.rsqrt(meansq + 1e-06) * norm_gain.astype(jnp.float32)[None, :]).astype(jnp.bfloat16)
    scaled = 2.5 * route_weights / lax.optimization_barrier(jnp.sum(route_weights, axis=1, keepdims=True))
    shared_out = swiglu(normed, shared_gate, shared_up, shared_down)
    capacity = max(2, TOK_DEV * TOP_K // N_EP + 1)
    route_blocks = routes.reshape(N_EP, TOK_DEV, TOP_K)
    weight_blocks = scaled.reshape(N_EP, TOK_DEV, TOP_K)
    x_blocks = normed.reshape(N_EP, TOK_DEV, D).astype(jnp.float32)

    def one_expert(carry, packed):
        gate_w, up_w, down_w, expert = packed
        select, weighted = expert_tables(route_blocks, weight_blocks, expert, capacity, EXPERTS)
        rows = jnp.einsum('stc,std->scd', select, x_blocks).astype(jnp.bfloat16)
        result = swiglu(rows.reshape(N_EP * capacity, D), gate_w, up_w, down_w).astype(jnp.bfloat16)
        result = result.reshape(N_EP, capacity, D).astype(jnp.float32)
        carry = carry + jnp.einsum('stc,scd->std', weighted, result, precision=lax.Precision.HIGHEST)
        return (carry, None)
    start = jnp.zeros((N_EP, TOK_DEV, D), jnp.float32)
    routed, _ = lax.scan(one_expert, start, (expert_gate, expert_up, expert_down, jnp.arange(EXPERTS, dtype=jnp.int32)))
    return (shared_out + routed.reshape(TOKENS, D)).astype(jnp.bfloat16)
```

```python
import functools

import jax
import jax.numpy as jnp
from jax import lax
from jax.experimental import pallas as pl
from jax.experimental.pallas import tpu as pltpu
from jax.sharding import PartitionSpec as P

MESH = pl.DeviceIdType.MESH
F32 = jnp.float32
BF16 = jnp.bfloat16
LANES = 128
TN = (((0,), (0,)), ((), ()))


def silu_mul(g, u):
    return g / (1.0 + jnp.exp(-g)) * u


def kernel(
    n, tp, cap, chunks, pieces,
    x_ref, gain_ref, routes_ref, rw_ref,
    eg_hbm, eu_hbm, ed_hbm, sg_hbm, su_hbm, sd_hbm,
    out_ref,
    wg, wu, wd, vg, vu, vd,
    packed, outbuf, arrive, retbuf, back,
    rows, mine, psend, precv, sssend, ssrecv, shsend, shrecv, acc, shout,
    wsem, dsend, drecv, rsend, rrecv, tsend, trecv, qsend, qrecv, hsend, hrecv,
):
    me = lax.axis_index("ep")
    my_tp = lax.axis_index("tp")
    toks, width = x_ref.shape
    picks = routes_ref.shape[1]
    ff = wg.shape[1]
    fs = vg.shape[1]
    blocks = width // LANES
    jc = blocks * cap
    n_rows = cap * n
    padded = shout.shape[0]
    cols = ff // chunks

    loads = {}
    slot = 0
    for name, src, dst in (
        ("sg", sg_hbm, vg), ("su", su_hbm, vu), ("sd", sd_hbm, vd),
        ("eg", eg_hbm.at[0], wg), ("eu", eu_hbm.at[0], wu), ("ed", ed_hbm.at[0], wd),
    ):
        depth = dst.shape[0] // pieces
        loads[name] = []
        for i in range(pieces):
            c = pltpu.make_async_copy(
                src.at[pl.ds(i * depth, depth)], dst.at[pl.ds(i * depth, depth)], wsem.at[slot]
            )
            c.start()
            loads[name].append(c)
            slot += 1

    barrier = pltpu.get_barrier_semaphore()
    order = sorted(range(1, n), key=lambda i: -min(i, n - i))
    for i in order:
        pl.semaphore_signal(barrier, inc=1, device_id={"ep": lax.rem(me + i, n)}, device_id_type=MESH)
    for i in range(1, tp):
        pl.semaphore_signal(barrier, inc=1, device_id={"tp": lax.rem(my_tp + i, tp)}, device_id_type=MESH)

    routes = routes_ref[...]
    rw = rw_ref[...]
    scaled = 2.5 * rw / jnp.sum(rw, axis=1, keepdims=True)
    lane_e = lax.broadcasted_iota(jnp.int32, (toks, n), 1)
    named = jnp.zeros((toks, n), F32)
    weight = jnp.zeros((toks, n), F32)
    for k in range(picks):
        hit = routes[:, k : k + 1] == lane_e
        named = named + jnp.where(hit, 1.0, 0.0)
        weight = weight + jnp.where(hit, scaled[:, k : k + 1], 0.0)
    row_i = lax.broadcasted_iota(jnp.int32, (toks, toks), 0)
    col_i = lax.broadcasted_iota(jnp.int32, (toks, toks), 1)
    lower = jnp.where(col_i < row_i, 1.0, 0.0)
    before = jnp.dot(lower, named, preferred_element_type=F32)
    place = jnp.where(named > 0.5, before, -1.0)
    spread_e = lax.broadcasted_iota(jnp.int32, (n, n_rows), 0)
    spread_c = lax.broadcasted_iota(jnp.int32, (n, n_rows), 1)
    spread = jnp.where(lax.rem(spread_c, n) == spread_e, 1.0, 0.0)
    place_x = jnp.dot(place, spread, preferred_element_type=F32)
    slot_x = (lax.broadcasted_iota(jnp.int32, (toks, n_rows), 1) // n).astype(F32)
    taken = place_x == slot_x
    w_hi = weight.astype(BF16).astype(F32)
    w_lo = (weight - w_hi).astype(BF16).astype(F32)
    comb_hi = jnp.where(taken, jnp.dot(w_hi, spread, preferred_element_type=F32), 0.0).astype(BF16)
    comb_lo = jnp.where(taken, jnp.dot(w_lo, spread, preferred_element_type=F32), 0.0).astype(BF16)
    select = jnp.where(taken, 1.0, 0.0).astype(BF16)

    def pack(value, j):
        for s in range(cap):
            packed[pl.ds(j * cap + s, n, stride=jc), :] = value[s * n : (s + 1) * n, :]

    def unpack(j):
        return jnp.concatenate(
            [packed[pl.ds(j * cap + s, n, stride=jc), :] for s in range(cap)], axis=0
        )

    x = x_ref[...]
    for j in range(blocks):
        cut = slice(j * LANES, (j + 1) * LANES)
        pack(lax.dot_general(select, x[:, cut], TN, preferred_element_type=F32), j)
    for p in range(n):
        outbuf[p] = packed[pl.ds(p * jc, jc), :].astype(BF16)

    pl.semaphore_wait(barrier, n - 1 + tp - 1)

    def exchange(src, dst, send, recv):
        copies = []
        for i in order:
            to = lax.rem(me + i, n)
            c = pltpu.make_async_remote_copy(
                src_ref=src.at[to], dst_ref=dst.at[me], send_sem=send.at[to], recv_sem=recv.at[me],
                device_id={"ep": to}, device_id_type=MESH,
            )
            c.start()
            copies.append(c)
        return copies

    def arrived(src, dst, send, recv):
        for i in order[::-1]:
            frm = lax.rem(me + i, n)
            pltpu.make_async_remote_copy(
                src_ref=src.at[frm], dst_ref=dst.at[frm], send_sem=send.at[frm], recv_sem=recv.at[frm],
                device_id={"ep": frm}, device_id_type=MESH,
            ).wait_recv()

    def to_tp(src, dst_of, send_of, recv_of):
        copies = []
        for i in range(1, tp):
            c = pltpu.make_async_remote_copy(
                src_ref=src, dst_ref=dst_of(i - 1), send_sem=send_of(i - 1), recv_sem=recv_of(i - 1),
                device_id={"tp": lax.rem(my_tp + i, tp)}, device_id_type=MESH,
            )
            c.start()
            copies.append(c)
        return copies

    pending = exchange(outbuf, arrive, dsend, drecv)
    arrive[me] = outbuf[me]

    xf = x.astype(F32)
    gain = gain_ref[...]
    xg = (xf * gain).astype(BF16)
    ss_own = jnp.sum(xf * xf, axis=1, keepdims=True)
    shsend[...] = jnp.zeros(shsend.shape, F32)
    shsend[0:toks, 2 * fs : 2 * fs + LANES] = jnp.broadcast_to(ss_own, (toks, LANES))
    for name, w, base in (("sg", vg, 0), ("su", vu, fs)):
        for c in loads[name]:
            c.wait()
        shsend[0:toks, base : base + fs] = jnp.dot(xg, w[...], preferred_element_type=F32)
    shcopies = to_tp(shsend, lambda i: shrecv.at[i], lambda i: hsend.at[i], lambda i: hrecv.at[i])
    pending += shcopies
    for name in ("sd", "eg", "eu", "ed"):
        for c in loads[name]:
            c.wait()
    for c in shcopies:
        c.wait_recv()
    total = shsend[...]
    for i in range(tp - 1):
        total = total + shrecv[i]
    r_own = lax.rsqrt(total[:, 2 * fs : 2 * fs + 1] / (width * tp) + 1e-06)
    sh_hidden = silu_mul(total[:, 0:fs] * r_own, total[:, fs : 2 * fs] * r_own).astype(BF16)
    shout[...] = jnp.dot(sh_hidden, vd[...], preferred_element_type=F32)

    arrived(outbuf, arrive, dsend, drecv)
    for p in range(n):
        packed[pl.ds(p * jc, jc), :] = arrive[p].astype(F32)
    ss = jnp.zeros((n_rows, LANES), F32)
    for j in range(blocks):
        cut = slice(j * LANES, (j + 1) * LANES)
        piece = unpack(j)
        ss = ss + piece * piece
        rows[:, cut] = (piece * gain[:, cut]).astype(BF16)
    sssend[...] = jnp.broadcast_to(jnp.sum(ss, axis=1, keepdims=True), (n_rows, LANES))
    sscopies = to_tp(sssend, lambda i: ssrecv.at[i], lambda i: qsend.at[i], lambda i: qrecv.at[i])
    pending += sscopies
    chunk_copies = []
    for c in range(chunks):
        cut = slice(c * cols, (c + 1) * cols)
        g = jnp.dot(rows[...], wg[:, cut], preferred_element_type=F32)
        u = jnp.dot(rows[...], wu[:, cut], preferred_element_type=F32)
        mine[c, :, 0:cols] = g
        mine[c, :, cols : 2 * cols] = u
        psend[c, :, 0:cols] = g.astype(BF16)
        psend[c, :, cols : 2 * cols] = u.astype(BF16)
        copies = to_tp(
            psend.at[c], lambda i: precv.at[i, c],
            lambda i: tsend.at[i * chunks + c], lambda i: trecv.at[i * chunks + c],
        )
        chunk_copies.append(copies)
        pending += copies
    for c in sscopies:
        c.wait_recv()
    ss_all = sssend[...]
    for i in range(tp - 1):
        ss_all = ss_all + ssrecv[i]
    r = lax.rsqrt(ss_all[:, 0:1] / (width * tp) + 1e-06)
    for c in range(chunks):
        for copy in chunk_copies[c]:
            copy.wait_recv()
        both = mine[c]
        for i in range(tp - 1):
            both = both + precv[i, c].astype(F32)
        hidden = silu_mul(both[:, 0:cols] * r, both[:, cols : 2 * cols] * r).astype(BF16)
        part = jnp.dot(hidden, wd[c * cols : (c + 1) * cols, :], preferred_element_type=F32)
        if c == 0:
            acc[...] = part
        elif c < chunks - 1:
            acc[...] += part
        else:
            for j in range(blocks):
                cut = slice(j * LANES, (j + 1) * LANES)
                pack(acc[:, cut] + part[:, cut], j)
    for p in range(n):
        retbuf[p] = packed[pl.ds(p * jc, jc), :].astype(BF16)
    pending += exchange(retbuf, back, rsend, rrecv)
    back[me] = retbuf[me]
    arrived(retbuf, back, rsend, rrecv)
    for p in range(n):
        packed[pl.ds(p * jc, jc), :] = back[p].astype(F32)
    for j in range(blocks):
        cut = slice(j * LANES, (j + 1) * LANES)
        piece = unpack(j).astype(BF16)
        routed = jnp.dot(comb_hi, piece, preferred_element_type=F32)
        routed = routed + jnp.dot(comb_lo, piece, preferred_element_type=F32)
        out_ref[:, cut] = (shout[0:toks, cut] + routed).astype(BF16)
    for c in pending:
        c.wait_send()


def local(tokens, norm_gain, routes, route_weights, eg, eu, ed, sg, su, sd):
    toks, width = tokens.shape
    picks = routes.shape[1]
    n, tp = lax.axis_size("ep"), lax.axis_size("tp")
    cap = max(2, toks * picks // n + 1)
    ff, fs = eg.shape[2], sg.shape[1]
    chunks, pieces = 4, 4
    jc = width // LANES * cap
    n_rows = n * cap
    padded = -(-toks // 16) * 16
    cols = ff // chunks
    others = max(1, tp - 1)
    vmem = pl.BlockSpec(memory_space=pltpu.VMEM)
    hbm = pl.BlockSpec(memory_space=pl.ANY)
    dma = pltpu.SemaphoreType.DMA
    return pl.pallas_call(
        functools.partial(kernel, n, tp, cap, chunks, pieces),
        out_shape=jax.ShapeDtypeStruct((toks, width), BF16),
        in_specs=[vmem] * 4 + [hbm] * 6,
        out_specs=vmem,
        scratch_shapes=[
            pltpu.VMEM((width, ff), BF16), pltpu.VMEM((width, ff), BF16), pltpu.VMEM((ff, width), BF16),
            pltpu.VMEM((width, fs), BF16), pltpu.VMEM((width, fs), BF16), pltpu.VMEM((fs, width), BF16),
            pltpu.VMEM((n * jc, LANES), F32),
            pltpu.VMEM((n, jc, LANES), BF16), pltpu.VMEM((n, jc, LANES), BF16),
            pltpu.VMEM((n, jc, LANES), BF16), pltpu.VMEM((n, jc, LANES), BF16),
            pltpu.VMEM((n_rows, width), BF16),
            pltpu.VMEM((chunks, n_rows, 2 * cols), F32),
            pltpu.VMEM((chunks, n_rows, 2 * cols), BF16),
            pltpu.VMEM((others, chunks, n_rows, 2 * cols), BF16),
            pltpu.VMEM((n_rows, LANES), F32), pltpu.VMEM((others, n_rows, LANES), F32),
            pltpu.VMEM((padded, 2 * fs + LANES), F32), pltpu.VMEM((others, padded, 2 * fs + LANES), F32),
            pltpu.VMEM((n_rows, width), F32), pltpu.VMEM((padded, width), F32),
            dma((6 * pieces,)),
            dma((n,)), dma((n,)), dma((n,)), dma((n,)),
            dma((others * chunks,)), dma((others * chunks,)),
            dma((others,)), dma((others,)), dma((others,)), dma((others,)),
        ],
        compiler_params=pltpu.CompilerParams(
            collective_id=0, has_side_effects=True, vmem_limit_bytes=60 * 1024 * 1024
        ),
    )(tokens, norm_gain.reshape(1, width), routes, route_weights, eg, eu, ed, sg, su, sd)


def solution(mesh):
    placed = (
        P("ep", "tp"),
        P("tp"),
        P("ep", None),
        P("ep", None),
        P("ep", "tp", None),
        P("ep", "tp", None),
        P("ep", None, "tp"),
        P("tp", None),
        P("tp", None),
        P(None, "tp"),
    )
    return jax.shard_map(
        local, mesh=mesh, in_specs=placed, out_specs=P("ep", "tp"), check_vma=False
    )
```

```python
import functools

import jax
import jax.numpy as jnp
from jax import lax
from jax.experimental import pallas as pl
from jax.experimental.pallas import tpu as pltpu
from jax.sharding import PartitionSpec as P

MESH = pl.DeviceIdType.MESH
F32 = jnp.float32
BF16 = jnp.bfloat16
LANES = 128
TN = (((0,), (0,)), ((), ()))
SPLIT = True
HILO = True


def silu_mul(g, u):
    return g / (1.0 + jnp.exp(-g)) * u


def kernel(
    n, tp, cap, chunks, pieces,
    x_ref, gain_ref, routes_ref, rw_ref,
    eg_hbm, eu_hbm, ed_hbm, sg_hbm, su_hbm, sd_hbm,
    out_ref,
    wg, wu, wd, vg, vu, vd,
    packed, outbuf, arrive, retbuf, back,
    rows, sssend, ssrecv, shsend, shrecv, acc, shout,
    wsem, dsend, drecv, rsend, rrecv, tsend, trecv, qsend, qrecv, hsend, hrecv,
    *exchanged,
):
    me = lax.axis_index("ep")
    my_tp = lax.axis_index("tp")
    toks, width = x_ref.shape
    picks = routes_ref.shape[0]
    ff = wg.shape[1]
    fs = vg.shape[1]
    blocks = width // LANES
    jc = blocks * cap
    n_rows = cap * n
    mine, psend, precv = exchanged[0::3], exchanged[1::3], exchanged[2::3]
    cols = ff // chunks

    barrier = pltpu.get_barrier_semaphore()
    for i in range(1, n):
        pl.semaphore_signal(barrier, inc=1, device_id={"ep": lax.rem(me + i, n)}, device_id_type=MESH)
    for i in range(1, tp):
        pl.semaphore_signal(barrier, inc=1, device_id={"tp": lax.rem(my_tp + i, tp)}, device_id_type=MESH)

    loads = {}
    slot = 0
    for name, src, dst in (
        ("sg", sg_hbm, vg), ("su", su_hbm, vu), ("sd", sd_hbm, vd),
        ("eg", eg_hbm.at[0], wg), ("eu", eu_hbm.at[0], wu), ("ed", ed_hbm.at[0], wd),
    ):
        depth = dst.shape[0] // pieces
        loads[name] = []
        for i in range(pieces):
            c = pltpu.make_async_copy(
                src.at[pl.ds(i * depth, depth)], dst.at[pl.ds(i * depth, depth)], wsem.at[slot]
            )
            c.start()
            loads[name].append(c)
            slot += 1

    routes = routes_ref[...]
    rw = rw_ref[...]
    scaled = 2.5 * rw / jnp.sum(rw, axis=0, keepdims=True)
    expert = lax.broadcasted_iota(jnp.int32, (n, toks), 0)
    named = jnp.zeros((n, toks), F32)
    weight = jnp.zeros((n, toks), F32)
    for k in range(picks):
        hit = routes[k : k + 1, :] == expert
        named = named + jnp.where(hit, 1.0, 0.0)
        weight = weight + jnp.where(hit, scaled[k : k + 1, :], 0.0)
    row_i = lax.broadcasted_iota(jnp.int32, (toks, toks), 0)
    col_i = lax.broadcasted_iota(jnp.int32, (toks, toks), 1)
    earlier = jnp.where(row_i < col_i, 1.0, 0.0).astype(BF16)
    before = jnp.dot(named.astype(BF16), earlier, preferred_element_type=F32)
    place = jnp.where(named > 0.5, before, -1.0)
    w_hi = weight.astype(BF16).astype(F32)
    w_lo = weight - w_hi

    def by_slot(v):
        return jnp.concatenate([jnp.where(place == s, v, 0.0) for s in range(cap)], axis=0).astype(BF16)

    select, comb_hi, comb_lo = by_slot(1.0), by_slot(w_hi), by_slot(w_lo)

    def pack(value, j, m):
        for s in range(cap):
            packed[pl.ds(j * cap + s, m, stride=jc), :] = value[s * m : (s + 1) * m, :]

    def unpack(j, m):
        return jnp.concatenate(
            [packed[pl.ds(j * cap + s, m, stride=jc), :] for s in range(cap)], axis=0
        )

    x = x_ref[...]
    for j in range(blocks):
        cut = slice(j * LANES, (j + 1) * LANES)
        pack(jnp.dot(select, x[:, cut], preferred_element_type=F32), j, n)
    for p in range(n):
        outbuf[p] = packed[pl.ds(p * jc, jc), :].astype(BF16)

    pl.semaphore_wait(barrier, n - 1 + tp - 1)

    def to_tp(src, dst_of, send_of, recv_of):
        copies = []
        for i in range(1, tp):
            c = pltpu.make_async_remote_copy(
                src_ref=src, dst_ref=dst_of(i - 1), send_sem=send_of(i - 1), recv_sem=recv_of(i - 1),
                device_id={"tp": lax.rem(my_tp + i, tp)}, device_id_type=MESH,
            )
            c.start()
            copies.append(c)
        return copies

    quarter = n // 4
    q, inner = me // quarter, lax.rem(me, quarter)
    half, bit = q // 2, lax.rem(q, 2)
    near = (q, 2 * half + 1 - bit)
    far = (2 * (1 - half) + bit, 2 * (1 - half) + 1 - bit)

    def members(quarters):
        return [qt * quarter + lax.rem(inner + i, quarter) for qt in quarters for i in range(quarter)]

    groups = [members(near)] + [members((f,)) for f in far] if SPLIT else [members(near), members(far)]

    def copy_to(src, dst, send, recv, to):
        return pltpu.make_async_remote_copy(
            src_ref=src.at[to], dst_ref=dst.at[me], send_sem=send.at[to], recv_sem=recv.at[me],
            device_id={"ep": to}, device_id_type=MESH,
        )

    def wait_from(src, dst, send, recv, frm):
        pltpu.make_async_remote_copy(
            src_ref=src.at[frm], dst_ref=dst.at[frm], send_sem=send.at[frm], recv_sem=recv.at[frm],
            device_id={"ep": frm}, device_id_type=MESH,
        ).wait_recv()

    pending = []

    def send_group(g, src, dst, send, recv):
        for i, to in enumerate(groups[g]):
            if g or i:
                c = copy_to(src, dst, send, recv, to)
                c.start()
                pending.append(c)

    def wait_group(g, src, dst, send, recv):
        for i, frm in enumerate(groups[g]):
            if g or i:
                wait_from(src, dst, send, recv, frm)

    for g in range(len(groups)):
        send_group(g, outbuf, arrive, dsend, drecv)
    arrive[me] = outbuf[me]

    xf = x.astype(F32)
    gain = gain_ref[...]
    xg = (xf * gain).astype(BF16)
    ss_own = jnp.sum(xf * xf, axis=1, keepdims=True)
    shsend[...] = jnp.zeros(shsend.shape, F32)
    shsend[0:toks, 2 * fs : 2 * fs + LANES] = jnp.broadcast_to(ss_own, (toks, LANES))
    for name, w, base in (("sg", vg, 0), ("su", vu, fs)):
        for c in loads[name]:
            c.wait()
        shsend[0:toks, base : base + fs] = jnp.dot(xg, w[...], preferred_element_type=F32)
    shcopies = to_tp(shsend, lambda i: shrecv.at[i], lambda i: hsend.at[i], lambda i: hrecv.at[i])
    pending.extend(shcopies)
    def finish_shared():
        for c in loads["sd"]:
            c.wait()
        for c in shcopies:
            c.wait_recv()
        total = shsend[...]
        for i in range(tp - 1):
            total = total + shrecv[i]
        r_own = lax.rsqrt(total[:, 2 * fs : 2 * fs + 1] / (width * tp) + 1e-06)
        sh_hidden = silu_mul(total[:, 0:fs] * r_own, total[:, fs : 2 * fs] * r_own).astype(BF16)
        shout[...] = jnp.dot(sh_hidden, vd[...], preferred_element_type=F32)

    def first_half(g):
        m = len(groups[g])
        count, base = m * cap, starts[g]
        low = -(-count // 16) * 16
        wait_group(g, outbuf, arrive, dsend, drecv)
        for i, p in enumerate(groups[g]):
            packed[pl.ds(i * jc, jc), :] = arrive[p].astype(F32)
        ss = jnp.zeros((count, LANES), F32)
        for j in range(blocks):
            cut = slice(j * LANES, (j + 1) * LANES)
            piece = unpack(j, m)
            ss = ss + piece * piece
            scaled_piece = piece * gain[:, cut]
            hi = scaled_piece.astype(BF16)
            rows[0:count, cut] = hi
            if HILO:
                rows[low : low + count, cut] = (scaled_piece - hi.astype(F32)).astype(BF16)
        sssend[base : base + count] = jnp.broadcast_to(jnp.sum(ss, axis=1, keepdims=True), (count, LANES))
        part = pl.ds(base, count)
        copies = to_tp(
            sssend.at[part], lambda i: ssrecv.at[i, part],
            lambda i: qsend.at[i * len(groups) + g], lambda i: qrecv.at[i * len(groups) + g],
        )
        all_copies = [copies]
        pending.extend(copies)
        taken_rows = rows[0 : 2 * low, :] if HILO else rows[0:count, :]
        for c in range(chunks):
            cut = slice(c * cols, (c + 1) * cols)
            for w, at in ((wg, 0), (wu, cols)):
                v = jnp.dot(taken_rows, w[:, cut], preferred_element_type=F32)
                if HILO:
                    v = v[0:count] + v[low : low + count]
                mine[g][c, :, at : at + cols] = v
                psend[g][c, :, at : at + cols] = v.astype(BF16)
            at_sem = lambda i: (i * len(groups) + g) * chunks + c
            copies = to_tp(
                psend[g].at[c], lambda i: precv[g].at[i, c],
                lambda i: tsend.at[at_sem(i)], lambda i: trecv.at[at_sem(i)],
            )
            all_copies.append(copies)
            pending.extend(copies)
        return all_copies

    def second_half(g, all_copies):
        m = len(groups[g])
        count, base = m * cap, starts[g]
        for c in all_copies[0]:
            c.wait_recv()
        ss_all = sssend[base : base + count, :]
        for i in range(tp - 1):
            ss_all = ss_all + ssrecv[i, base : base + count, :]
        r = lax.rsqrt(ss_all[:, 0:1] / (width * tp) + 1e-06)
        for c in range(chunks):
            for copy in all_copies[1 + c]:
                copy.wait_recv()
            both = mine[g][c]
            for i in range(tp - 1):
                both = both + precv[g][i, c].astype(F32)
            hidden = silu_mul(both[:, 0:cols] * r, both[:, cols : 2 * cols] * r).astype(BF16)
            part = jnp.dot(hidden, wd[c * cols : (c + 1) * cols, :], preferred_element_type=F32)
            if c == 0:
                acc[0:count, :] = part
            elif c < chunks - 1:
                acc[0:count, :] += part
            else:
                for j in range(blocks):
                    cut = slice(j * LANES, (j + 1) * LANES)
                    pack(acc[0:count, cut] + part[:, cut], j, m)
        for i, p in enumerate(groups[g]):
            retbuf[p] = packed[pl.ds(i * jc, jc), :].astype(BF16)
        send_group(g, retbuf, back, rsend, rrecv)

    starts = []
    for g in range(len(groups)):
        starts.append(sum(-(-len(groups[i]) * cap // 8) * 8 for i in range(g)))
    if HILO:
        rows[...] = jnp.zeros(rows.shape, BF16)
    for name in ("eg", "eu"):
        for c in loads[name]:
            c.wait()
    states = [first_half(0)]
    finish_shared()
    for c in loads["ed"]:
        c.wait()
    if len(groups) == 3:
        states.append(first_half(1))
        second_half(0, states[0])
        states.append(first_half(2))
    else:
        states.append(first_half(1))
        second_half(0, states[0])
    back[me] = retbuf[me]
    for g in range(1, len(groups)):
        second_half(g, states[g])
    for g in range(len(groups)):
        wait_group(g, retbuf, back, rsend, rrecv)
    for p in range(n):
        packed[pl.ds(p * jc, jc), :] = back[p].astype(F32)
    for j in range(blocks):
        cut = slice(j * LANES, (j + 1) * LANES)
        piece = unpack(j, n).astype(BF16)
        routed = lax.dot_general(comb_hi, piece, TN, preferred_element_type=F32)
        routed = routed + lax.dot_general(comb_lo, piece, TN, preferred_element_type=F32)
        out_ref[:, cut] = (shout[0:toks, cut] + routed).astype(BF16)
    for c in pending:
        c.wait_send()


def local(tokens, norm_gain, routes, route_weights, eg, eu, ed, sg, su, sd):
    toks, width = tokens.shape
    picks = routes.shape[1]
    n, tp = lax.axis_size("ep"), lax.axis_size("tp")
    cap = max(2, toks * picks // n + 1)
    ff, fs = eg.shape[2], sg.shape[1]
    chunks, pieces = 2, 4
    jc = width // LANES * cap
    n_rows = n * cap
    padded = -(-toks // 16) * 16
    cols = ff // chunks
    others = max(1, tp - 1)
    sizes = [n // 2, n // 4, n // 4] if SPLIT else [n // 2, n // 2]
    exchanged = []
    for m in sizes:
        exchanged += [
            pltpu.VMEM((chunks, m * cap, 2 * cols), F32),
            pltpu.VMEM((chunks, m * cap, 2 * cols), BF16),
            pltpu.VMEM((others, chunks, m * cap, 2 * cols), BF16),
        ]
    vmem = pl.BlockSpec(memory_space=pltpu.VMEM)
    hbm = pl.BlockSpec(memory_space=pl.ANY)
    dma = pltpu.SemaphoreType.DMA
    return pl.pallas_call(
        functools.partial(kernel, n, tp, cap, chunks, pieces),
        out_shape=jax.ShapeDtypeStruct((toks, width), BF16),
        in_specs=[vmem] * 4 + [hbm] * 6,
        out_specs=vmem,
        scratch_shapes=[
            pltpu.VMEM((width, ff), BF16), pltpu.VMEM((width, ff), BF16), pltpu.VMEM((ff, width), BF16),
            pltpu.VMEM((width, fs), BF16), pltpu.VMEM((width, fs), BF16), pltpu.VMEM((fs, width), BF16),
            pltpu.VMEM((n * jc, LANES), F32),
            pltpu.VMEM((n, jc, LANES), BF16), pltpu.VMEM((n, jc, LANES), BF16),
            pltpu.VMEM((n, jc, LANES), BF16), pltpu.VMEM((n, jc, LANES), BF16),
            pltpu.VMEM((2 * n_rows, width), BF16),
            pltpu.VMEM((2 * n_rows, LANES), F32), pltpu.VMEM((others, 2 * n_rows, LANES), F32),
            pltpu.VMEM((padded, 2 * fs + LANES), F32), pltpu.VMEM((others, padded, 2 * fs + LANES), F32),
            pltpu.VMEM((n_rows, width), F32), pltpu.VMEM((padded, width), F32),
            dma((6 * pieces,)),
            dma((n,)), dma((n,)), dma((n,)), dma((n,)),
            dma((others * chunks * len(sizes),)), dma((others * chunks * len(sizes),)),
            dma((others * len(sizes),)), dma((others * len(sizes),)), dma((others,)), dma((others,)),
        ] + exchanged,
        compiler_params=pltpu.CompilerParams(
            collective_id=0, has_side_effects=True, vmem_limit_bytes=60 * 1024 * 1024
        ),
    )(tokens, norm_gain.reshape(1, width), routes.T, route_weights.T, eg, eu, ed, sg, su, sd)


def solution(mesh):
    placed = (
        P("ep", "tp"),
        P("tp"),
        P("ep", None),
        P("ep", None),
        P("ep", "tp", None),
        P("ep", "tp", None),
        P("ep", None, "tp"),
        P("tp", None),
        P("tp", None),
        P(None, "tp"),
    )
    return jax.shard_map(
        local, mesh=mesh, in_specs=placed, out_specs=P("ep", "tp"), check_vma=False
    )
```
